32 devices in a mesh: dp: 4 (over y, x), kv: 4 (over z), tp: 2 (over core).
Axes of the slice: x: 2, y: 2, z: 4, core: 2. Of those that a mesh axis runs over, the one named last changes fastest.
Arguments:
- tokens: bfloat16 [32, 2048], P('dp', 'kv'), may hold values from -6 to 6
- pre_gain: float32 [2048], P('kv'), may hold values from 0.1 to 1.9
- query_weight: bfloat16 [2048, 1024], P('kv', 'tp'), may hold values from -0.125 to 0.125
- key_weight: bfloat16 [2048, 1024], P('kv', 'tp'), may hold values from -0.125 to 0.125
- value_weight: bfloat16 [2048, 1024], P('kv', 'tp'), may hold values from -0.125 to 0.125
- outgate_weight: bfloat16 [2048, 1024], P('kv', 'tp'), may hold values from -0.125 to 0.125
- input_gate_weight: bfloat16 [2048, 4], replicated, may hold values from -0.125 to 0.125
- forget_gate_weight: bfloat16 [2048, 4], replicated, may hold values from -0.125 to 0.125
- cache_keys: bfloat16 [32, 64, 1024], P(('dp', 'kv'), None, 'tp'), may hold values from -6 to 6
- cache_values: bfloat16 [32, 64, 1024], P(('dp', 'kv'), None, 'tp'), may hold values from -6 to 6
- cache_input: float32 [32, 64, 4], P(('dp', 'kv'), None, 'tp'), may hold values from -6 to 250
- cache_forget: float32 [32, 64, 4], P(('dp', 'kv'), None, 'tp'), may hold values from -0.7 to 0
- lengths: int32 [32], P(('dp', 'kv')), may hold values from 1 to 64, 819 in all
- state_matrix: float32 [32, 4, 256, 256], P(('dp', 'kv'), 'tp'), may hold values from -6 to 6
- state_norm: float32 [32, 4, 256], P(('dp', 'kv'), 'tp'), may hold values from -6 to 6
- state_max: float32 [32, 4], P(('dp', 'kv'), 'tp'), may hold values from -4 to 253
- head_gain: float32 [1024], P('tp'), may hold values from 0.1 to 1.9
- out_weight: bfloat16 [1024, 2048], P('tp', 'kv'), may hold values from -0.375 to 0.375
- mixer_gain: float32 [2048], replicated, may hold values from 0.1 to 1.9
- gate_weight: bfloat16 [2048, 5632], P(None, ('kv', 'tp')), may hold values from -0.125 to 0.125
- up_weight: bfloat16 [2048, 5632], P(None, ('kv', 'tp')), may hold values from -0.125 to 0.125
- down_weight: bfloat16 [5632, 2048], P(('kv', 'tp')), may hold values from -0.21875 to 0.21875
Outputs:
- layer_out: bfloat16 [32, 2048], P('dp', ('kv', 'tp'))
The draws below stay inside these ranges and needn't reach their ends.
Inputs may be any that keep to these rules, and one draw needn't show every extreme that they name: `lengths`: positions from a sequence's length on take no part.
All inputs are finite; a program needn't handle non-finite values. No bound on the sum of `lengths` on one device may be relied on, other than what follows from the above.
Results may differ from the reference program's by a relative error of at most 0.018.
Values may be sent and summed in bfloat16 or wider, within the bound.
No kernel may reach another device: no remote copies, remote signals or barrier semaphores. Data moves between devices by JAX's collectives and lax.ppermute only.
A program may use at most 64 MiB of HBM per device.

```python
import math
import jax
import jax.numpy as jnp
import numpy as np
from jax import lax

D = 2048
MEMORY_HEADS = 4
HEAD_DIM = 256
FF = 5632
FOLD_SPAN = 64
HW = 1024
SEQUENCE_TOTAL = 32
N_TP = 2


def draw_cache_input(key, part):
    noise = jnp.clip(jax.random.normal(jax.random.fold_in(key, 11), (SEQUENCE_TOTAL, FOLD_SPAN, MEMORY_HEADS), jnp.float32), -6.0, 6.0)
    return noise


def draw_state_max(key, part):
    noise = jnp.clip(jax.random.normal(jax.random.fold_in(key, 13), (SEQUENCE_TOTAL, MEMORY_HEADS), jnp.float32), -4.0, 4.0)
    return noise


def draw_cache_forget(key, part):
    divided_random_keys = jax.random.split(jax.random.fold_in(key, 17), 6)
    fast_share = 0.5
    fast = jax.random.bernoulli(divided_random_keys[0], fast_share, (SEQUENCE_TOTAL, MEMORY_HEADS))
    fast_rate = jax.random.uniform(divided_random_keys[1], (SEQUENCE_TOTAL, MEMORY_HEADS), jnp.float32, math.log(10.0) / 50.0, math.log(10.0) / 30.0)
    slow_rate = jax.random.uniform(divided_random_keys[2], (SEQUENCE_TOTAL, MEMORY_HEADS), jnp.float32, 0.1, 0.8) * (math.log(10.0) / FOLD_SPAN)
    rate = jnp.where(fast, fast_rate, slow_rate)
    jitter = jax.random.uniform(divided_random_keys[3], (SEQUENCE_TOTAL, FOLD_SPAN, MEMORY_HEADS), jnp.float32, 0.5, 1.5)
    retain_logarithm = -rate[:, None, :] * jitter
    sudden_spike = jax.random.bernoulli(divided_random_keys[4], 3.0 / FOLD_SPAN, (SEQUENCE_TOTAL, FOLD_SPAN, MEMORY_HEADS))
    discarded_entries = jnp.log(jax.random.uniform(divided_random_keys[5], (SEQUENCE_TOTAL, FOLD_SPAN, MEMORY_HEADS), jnp.float32, 0.5, 0.8))
    return jnp.where(sudden_spike, discarded_entries, retain_logarithm)


def spiked(values, key, source, target, blocks, factor):
    owner, partner = [(jnp.arange(values.shape[position]) // (values.shape[position] // blocks)).reshape([-1 if axis == position else 1 for axis in range(values.ndim)]) for position in (source, target)]
    chosen = jax.random.permutation(key, blocks)[partner]
    strong = (owner == chosen) | (owner == (partner + blocks // 2) % blocks)
    return jnp.where(strong, factor * values, values)


def block_levels(stream_key, shape, cuts, low, largest):
    level = 1.0
    for axis_at, blocks in cuts:
        draws = jax.random.uniform(jax.random.fold_in(jax.random.fold_in(stream_key, 6), axis_at), (blocks,), jnp.float32, low / len(cuts), largest / len(cuts))
        level = level * jnp.repeat(jnp.exp(draws), shape[axis_at] // blocks).reshape((-1,) + (1,) * (len(shape) - 1 - axis_at))
    return level


def split_up(number_of, total, limit, slope):
    weights = [(1 << 20) // math.isqrt(grade ** slope) + 1 for grade in range(2, number_of + 1)]
    surplus, counts = total - limit - (number_of - 1), [1] * (number_of - 1)
    while surplus > 0:
        candidates = [i for i in range(number_of - 1) if counts[i] < limit]
        whole, remaining = sum([weights[i] for i in candidates]), surplus
        for i in candidates:
            addition = min(limit - counts[i], max(1, remaining * weights[i] // whole), surplus)
            counts[i] = counts[i] + addition
            surplus = surplus - addition
    return np.array([limit] + counts)


def ragged_sizes(own_key, amount, total, most, slope):
    if amount == 2:
        one = jax.random.randint(own_key, (), max(1, total - most), min(most, total - 1) + 1)
        return jnp.stack([one, total - one])
    sizes = jnp.asarray(split_up(amount, total, most, slope), jnp.int32)
    twos = (amount - 1) // 2
    donor, sink = sizes[1:1 + 2 * twos:2], sizes[2:2 + 2 * twos:2]
    room = jnp.minimum(donor - 1, most - sink)
    moved = jax.random.randint(jax.random.fold_in(own_key, 1), (twos,), 0, 1 << 20) % (room + 1)
    sizes = sizes.at[1:1 + 2 * twos:2].set(donor - moved).at[2:2 + 2 * twos:2].set(sink + moved)
    return sizes[jax.random.permutation(jax.random.fold_in(own_key, 2), amount)]


def gaussian(rng, extent, scale, reach, cuts=(), kind=jnp.bfloat16):
    level = block_levels(rng, extent, cuts, -0.22, 0.18) if cuts else 1.0
    result = jax.random.normal(rng, extent, jnp.float32) * scale * level
    return jnp.minimum(jnp.maximum(result, -reach), reach).astype(kind)


def gaussian_with(key, extent, spread, reach, cuts, heavy, held_as=jnp.bfloat16):
    array = spread * jax.random.normal(key, extent, jnp.float32)
    if cuts:
        array = array * block_levels(key, extent, cuts, -0.22, 0.18)
    return jnp.clip(spiked(array, jax.random.fold_in(key, 3), *heavy), -reach, reach).astype(held_as)


def setup_inputs(seed: int = 0) -> dict:
    key_of = jax.random.split(jax.random.key(seed), 23)
    return {
        "tokens": gaussian_with(key_of[0], (SEQUENCE_TOTAL, D), 1.0, 6.0, ((0, 4), (1, 4)), (1, 0, 4, 2.0)),
        "pre_gain": jnp.clip(1.0 + 0.18 * jax.random.normal(key_of[1], (D,), jnp.float32), 0.1, 1.9),
        "query_weight": gaussian(key_of[2], (D, HW), D ** -0.5, 0.125, ((0, 4), (1, 2))),
        "key_weight": gaussian(key_of[3], (D, HW), D ** -0.5, 0.125, ((0, 4), (1, 2))),
        "value_weight": gaussian(key_of[4], (D, HW), D ** -0.5, 0.125, ((0, 4), (1, 2))),
        "outgate_weight": gaussian(key_of[5], (D, HW), D ** -0.5, 0.125, ((0, 4), (1, 2))),
        "input_gate_weight": gaussian(key_of[6], (D, MEMORY_HEADS), D ** -0.5, 0.125),
        "forget_gate_weight": gaussian(key_of[7], (D, MEMORY_HEADS), D ** -0.5, 0.125),
        "cache_keys": gaussian(key_of[8], (SEQUENCE_TOTAL, FOLD_SPAN, HW), 1.0, 6.0, ((0, 16), (2, 2))),
        "cache_values": gaussian(key_of[9], (SEQUENCE_TOTAL, FOLD_SPAN, HW), 1.0, 6.0, ((0, 16), (2, 2))),
        "cache_input": draw_cache_input(jax.random.fold_in(key_of[22], 71), 0),
        "cache_forget": draw_cache_forget(jax.random.fold_in(key_of[22], 71), 0),
        "lengths": ragged_sizes(key_of[12], SEQUENCE_TOTAL, SEQUENCE_TOTAL * FOLD_SPAN * 2 // 5, FOLD_SPAN, 2).astype(jnp.int32),
        "state_matrix": gaussian(key_of[13], (SEQUENCE_TOTAL, MEMORY_HEADS, HEAD_DIM, HEAD_DIM), 1.0, 6.0, ((0, 16), (1, 2)), jnp.float32),
        "state_norm": gaussian(key_of[14], (SEQUENCE_TOTAL, MEMORY_HEADS, HEAD_DIM), 1.0, 6.0, ((0, 16), (1, 2)), jnp.float32),
        "state_max": draw_state_max(jax.random.fold_in(key_of[22], 71), 0),
        "head_gain": jnp.clip(1.0 + 0.18 * jax.random.normal(key_of[16], (HW,), jnp.float32), 0.1, 1.9),
        "out_weight": gaussian(key_of[17], (HW, D), (HW // 4) ** -0.5, 0.375, ((0, 2), (1, 4))),
        "mixer_gain": jnp.clip(1.0 + 0.18 * jax.random.normal(key_of[18], (D,), jnp.float32), 0.1, 1.9),
        "gate_weight": gaussian(key_of[19], (D, FF), D ** -0.5, 0.125, ((1, 8),)),
        "up_weight": gaussian(key_of[20], (D, FF), D ** -0.5, 0.125, ((1, 8),)),
        "down_weight": gaussian_with(key_of[21], (FF, D), (FF // 4) ** -0.5, 0.21875, ((0, 8),), (0, 1, 8, 2.0)),
    }


EPS = 1e-06

def reference(tokens, pre_gain, query_weight, key_weight, value_weight, outgate_weight, input_gate_weight, forget_gate_weight, cache_keys, cache_values, cache_input, cache_forget, lengths, state_matrix, state_norm, state_max, head_gain, out_weight, mixer_gain, gate_weight, up_weight, down_weight):
    token_values = tokens.astype(jnp.float32)
    scale_first = lax.rsqrt(lax.optimization_barrier(jnp.mean(token_values * token_values, axis=1)) + EPS)[:, None]
    normed_first = (token_values * pre_gain[None, :]).astype(jnp.bfloat16)

    def project(weight):
        return scale_first * jnp.dot(normed_first, weight, preferred_element_type=jnp.float32)
    query = project(query_weight).astype(jnp.bfloat16)
    keys_new = project(key_weight).astype(jnp.bfloat16)
    values_new = project(value_weight).astype(jnp.bfloat16)
    outgate = project(outgate_weight).astype(jnp.bfloat16)
    in_gate = project(input_gate_weight)
    forget_new = jax.nn.log_sigmoid(project(forget_gate_weight))
    seq_count = tokens.shape[0]
    query_heads = query.astype(jnp.float32).reshape(seq_count, MEMORY_HEADS, HEAD_DIM) * HEAD_DIM ** (-0.5)
    key_heads = keys_new.astype(jnp.float32).reshape(seq_count, MEMORY_HEADS, HEAD_DIM)
    value_heads = values_new.astype(jnp.float32).reshape(seq_count, MEMORY_HEADS, HEAD_DIM)
    cached_keys = cache_keys.astype(jnp.float32).reshape(seq_count, FOLD_SPAN, MEMORY_HEADS, HEAD_DIM)
    cached_values = cache_values.astype(jnp.float32).reshape(seq_count, FOLD_SPAN, MEMORY_HEADS, HEAD_DIM)
    live_mask = (jnp.arange(FOLD_SPAN, dtype=jnp.int32)[None, :] < lengths[:, None])[:, :, None]
    forget_live = jnp.where(live_mask, cache_forget, jnp.float32(0.0))
    running = jnp.cumsum(forget_live, axis=1)
    total_log = running[:, -1, :] + forget_new
    weight_log = jnp.where(live_mask, total_log[:, None, :] - running + cache_input, -jnp.inf)
    state_log = total_log + state_max
    peak_log = jnp.maximum(jnp.maximum(state_log, in_gate), lax.optimization_barrier(jnp.max(weight_log, axis=1)))
    key_dots = jnp.einsum('bhd,blhd->blh', query_heads, cached_keys)
    block_scores = jnp.exp(weight_log - peak_log[:, None, :]) * key_dots
    self_score = jnp.exp(in_gate - peak_log) * lax.optimization_barrier(jnp.sum(query_heads * key_heads, axis=2))
    carried = jnp.exp(state_log - peak_log)
    block_weights = lax.optimization_barrier(block_scores.astype(jnp.bfloat16)).astype(jnp.float32)
    memory_read = jnp.einsum('bhvd,bhd->bhv', state_matrix, query_heads, precision=lax.Precision.HIGHEST)
    norm_read = jnp.einsum('bhd,bhd->bh', state_norm, query_heads, precision=lax.Precision.HIGHEST)
    numerator = carried[:, :, None] * memory_read + jnp.einsum('blh,blhd->bhd', block_weights, cached_values) + self_score[:, :, None] * value_heads
    denominator = carried * norm_read + lax.optimization_barrier(jnp.sum(block_scores, axis=1)) + self_score
    hidden = numerator / jnp.maximum(jnp.abs(denominator), 1.0)[:, :, None]
    mixed_heads = (hidden.reshape(seq_count, HW) * head_gain[None, :] * jax.nn.sigmoid(outgate.astype(jnp.float32))).astype(jnp.bfloat16)
    half_width = HW // N_TP
    mix_sum = jnp.zeros((seq_count, D), jnp.float32)
    for half_part in range(N_TP):
        piece_sum = jnp.dot(mixed_heads[:, half_part * half_width:(half_part + 1) * half_width], out_weight[half_part * half_width:(half_part + 1) * half_width], preferred_element_type=jnp.float32)
        mix_sum = mix_sum + lax.optimization_barrier(piece_sum.astype(jnp.bfloat16)).astype(jnp.float32)
    residual = (token_values + mix_sum).astype(jnp.bfloat16)
    residual_values = residual.astype(jnp.float32)
    scale_mid = lax.rsqrt(lax.optimization_barrier(jnp.mean(residual_values * residual_values, axis=1)) + EPS)[:, None]
    normed_mid = (residual_values * mixer_gain[None, :]).astype(jnp.bfloat16)
    gate_values = scale_mid * jnp.dot(normed_mid, gate_weight, preferred_element_type=jnp.float32)
    up_values = scale_mid * jnp.dot(normed_mid, up_weight, preferred_element_type=jnp.float32)
    hidden_units = (jax.nn.silu(gate_values) * up_values).astype(jnp.bfloat16)
    return (residual_values + jnp.dot(hidden_units, down_weight, preferred_element_type=jnp.float32)).astype(jnp.bfloat16)
```

```python
import jax
import jax.numpy as jnp
from jax import lax
from jax.experimental import pallas as pl
from jax.experimental.pallas import tpu as pltpu
from jax.sharding import PartitionSpec as P

EPS = 1e-06
LANES = 128
COVER = 6_000_000_000
VMEM = pl.BlockSpec(memory_space=pltpu.VMEM)
HBM = pl.BlockSpec(memory_space=pltpu.HBM)
F32 = jnp.float32
BF16 = jnp.bfloat16


def dot(a, b, dims=((1,), (0,))):
    return lax.dot_general(a, b, (dims, ((), ())), preferred_element_type=F32)


def fetch(sources, targets, sems):
    copies = [
        pltpu.make_async_copy(source, target, sems.at[n])
        for n, (source, target) in enumerate(zip(sources, targets))
    ]
    for copy in copies:
        copy.start()
    return copies


def cost(flops):
    return pl.CostEstimate(flops=flops, bytes_accessed=0, transcendentals=0)


def grant(mebibytes):
    return pltpu.CompilerParams(vmem_limit_bytes=mebibytes * 2**20)


def xor_swap(value, step, count):
    return lax.ppermute(value, "kv", [(i, i ^ step) for i in range(count)])


def marker_kernel(mark, *, lane_at):
    lane = lax.broadcasted_iota(jnp.int32, mark.shape, 1)
    mark[...] = jnp.where(lane == lane_at, 1.0, 0.0)


def project_kernel(
    mark, tokens, gain, wq, wk, wv, wo, wi, wf, *rest, kv_count, own_seqs, gate_count
):
    outs = rest[:kv_count]
    token_buf, gain_buf, bufs, gate_bufs, acc, sems = rest[kv_count:]
    rows, width = tokens.shape
    cols = wq.shape[1]
    me = lax.axis_index("kv")
    here = pl.ds(pl.multiple_of(me * width, width), width)
    sources = (tokens, gain, wi.at[:, here], wf.at[:, here], wq, wk, wv, wo)
    targets = (token_buf, gain_buf, gate_bufs.at[0], gate_bufs.at[1], *[bufs.at[n] for n in range(4)])
    copies = fetch(sources, targets, sems)
    copies[0].wait()
    copies[1].wait()
    values = token_buf[...].astype(F32)
    squares = jnp.sum(values * values, axis=1, keepdims=True)
    normed = (values * gain_buf[...]).astype(BF16)
    extra = mark[...] * squares

    def put(start, part):
        for k in range(kv_count):
            acc[k, :, start : start + part.shape[1]] = part[k * own_seqs : (k + 1) * own_seqs, :]

    put(4 * cols, extra)
    for n in range(4):
        copies[4 + n].wait()
        put(n * cols, dot(normed, bufs[n]))
    for n in range(2):
        copies[2 + n].wait()
        put(4 * cols + n * gate_count, dot(normed, gate_bufs[n], ((1,), (1,))))
    for step in range(kv_count):
        outs[step][...] = acc[me ^ step]


def cell_kernel(
    *refs, kv_count, model_width, head_count, gate_count
):
    parts = refs[:kv_count]
    sources = refs[kv_count : kv_count + 9]
    out = refs[kv_count + 9]
    buffers = refs[kv_count + 10 : kv_count + 19]
    copies = fetch(sources, buffers, refs[kv_count + 19])
    (cache_input, cache_forget, lengths, norm, peak, gain, keys, state, values) = buffers
    own_seqs, block_len, cols = keys.shape
    head_size = cols // head_count
    half = lax.axis_index("tp")
    inv_root = head_size ** (-0.5)
    total = parts[0][...]
    for part in parts[1:]:
        total = total + part[...]
    extra = total[:, 4 * cols :]
    squares = extra[:, 2 * gate_count : 2 * gate_count + 1]
    scale = lax.rsqrt(squares / model_width + EPS)
    query, key_new, value_new, outgate = [
        (scale * total[:, n * cols : (n + 1) * cols]).astype(BF16) for n in range(4)
    ]
    gates = scale * extra

    lane_head = lax.broadcasted_iota(jnp.int32, (head_count, cols), 1) // head_size
    own_lane = lane_head == lax.broadcasted_iota(jnp.int32, (head_count, cols), 0)
    upper = (
        lax.broadcasted_iota(jnp.int32, (block_len, block_len), 0)
        <= lax.broadcasted_iota(jnp.int32, (block_len, block_len), 1)
    ).astype(F32)
    position = lax.broadcasted_iota(jnp.int32, (head_count, block_len), 1)

    def column(row, start):
        shape = (head_count, row.shape[1])
        at = lax.broadcasted_iota(jnp.int32, shape, 0) + start
        picked = jnp.where(lax.broadcasted_iota(jnp.int32, shape, 1) == at, row, 0.0)
        return jnp.sum(picked, axis=1, keepdims=True)


    def spread(per_head):
        return jnp.sum(jnp.where(own_lane, per_head, 0.0), axis=0, keepdims=True)

    for copy in copies:
        copy.wait()
    for s in range(own_seqs):
        live = position < lengths[:, s : s + 1]
        forget_live = jnp.where(live, cache_forget[s], 0.0)
        running = lax.dot_general(
            forget_live,
            upper,
            (((1,), (0,)), ((), ())),
            precision=lax.Precision.HIGHEST,
            preferred_element_type=F32,
        )
        gates_s = gates[s : s + 1]
        gate_s = column(gates_s, half * head_count)
        forget_new = jax.nn.log_sigmoid(column(gates_s, gate_count + half * head_count))
        total_log = running[:, block_len - 1 : block_len] + forget_new
        weight_log = jnp.where(live, total_log - running + cache_input[s], -jnp.inf)
        state_log = total_log + column(peak[s : s + 1], 0)
        peak_log = jnp.maximum(
            jnp.maximum(state_log, gate_s), jnp.max(weight_log, axis=1, keepdims=True)
        )
        query_s = query[s : s + 1].astype(F32)
        query_rows = jnp.where(own_lane, query_s, 0.0)
        key_dots = dot(query_rows.astype(BF16), keys[s], ((1,), (1,))) * inv_root
        scores = jnp.exp(weight_log - peak_log) * key_dots
        query_rows = query_rows * inv_root
        self_dot = jnp.sum(query_rows * key_new[s : s + 1].astype(F32), axis=1, keepdims=True)
        read = dot(scores.astype(BF16), values[s])
        read = jnp.sum(jnp.where(own_lane, read, 0.0), axis=0, keepdims=True)
        memory, norm_dot = [], []
        for h in range(head_count):
            at = slice(h * head_size, (h + 1) * head_size)
            matrix = state[s, h]
            high = matrix.astype(BF16)
            low = (matrix - high.astype(F32)).astype(BF16)
            query_h = query_s[:, at].astype(BF16)
            memory.append(dot(query_h, high, ((1,), (1,))) + dot(query_h, low, ((1,), (1,))))
            norm_dot.append(
                jnp.sum(query_s[:, at] * norm[s, h : h + 1, :], axis=1, keepdims=True)
            )
        memory = jnp.concatenate(memory, axis=1) * inv_root
        norm_dot = jnp.concatenate(norm_dot, axis=0) * inv_root
        self_score = jnp.exp(gate_s - peak_log) * self_dot
        carried = jnp.exp(state_log - peak_log)
        numerator = (
            spread(carried) * memory + read + spread(self_score) * value_new[s : s + 1].astype(F32)
        )
        denominator = carried * norm_dot + jnp.sum(scores, axis=1, keepdims=True) + self_score
        hidden = numerator / spread(jnp.maximum(jnp.abs(denominator), 1.0))
        gated = hidden * gain[...] * jax.nn.sigmoid(outgate[s : s + 1].astype(F32))
        out[s : s + 1, :] = gated.astype(BF16)


def mix_kernel(*refs, kv_count):
    parts = refs[:kv_count]
    weight, product, ordered = refs[kv_count:]
    me = lax.axis_index("kv")
    for step in range(kv_count):
        ordered[me ^ step] = parts[step][...].astype(F32)
    heads = jnp.concatenate([ordered[k] for k in range(kv_count)], axis=0).astype(BF16)
    product[...] = dot(heads, weight[...]).astype(BF16)


def mixer_kernel(*refs, kv_count, model_width):
    parts = refs[:kv_count]
    gain, wg, wu, wd, sent, ordered = refs[kv_count:]
    rows, width = parts[0].shape
    narrow = sent.shape[2]
    me = lax.axis_index("kv")
    squares = jnp.zeros((rows, 1), F32)
    for step in range(kv_count):
        wide = parts[step][...].astype(F32)
        squares = squares + jnp.sum(wide * wide, axis=1, keepdims=True)
        ordered[me ^ step] = wide
    normed = jnp.concatenate(
        [ordered[k] * gain[:, k * width : (k + 1) * width] for k in range(kv_count)], axis=1
    ).astype(BF16)
    scale = lax.rsqrt(squares / model_width + EPS)
    gate = scale * dot(normed, wg[...], ((1,), (1,)))
    up = scale * dot(normed, wu[...], ((1,), (1,)))
    units = (jax.nn.silu(gate) * up).astype(BF16)
    for k in range(sent.shape[0]):
        sent[k] = dot(units, wd[:, k * narrow : (k + 1) * narrow])


def aligned_device(
    tokens,
    pre_gain,
    query_weight,
    key_weight,
    value_weight,
    outgate_weight,
    input_gate_weight,
    forget_gate_weight,
    cache_keys,
    cache_values,
    cache_input,
    cache_forget,
    lengths,
    state_matrix,
    state_norm,
    state_max,
    head_gain,
    out_weight,
    mixer_gain,
    gate_weight,
    up_weight,
    down_weight,
):
    kv_count = lax.axis_size("kv")
    tp_count = lax.axis_size("tp")
    rows, width = tokens.shape
    own_seqs = cache_keys.shape[0]
    cols = query_weight.shape[1]
    head_count = state_max.shape[1]
    gate_count = input_gate_weight.shape[1]
    model_width = width * kv_count
    group = kv_count * tp_count
    narrow = width // tp_count
    packed = 4 * cols + LANES
    mark = pl.pallas_call(
        lambda ref: marker_kernel(ref, lane_at=2 * gate_count),
        name="marker",
        out_specs=VMEM,
        out_shape=jax.ShapeDtypeStruct((rows, LANES), F32),
        compiler_params=grant(1),
        cost_estimate=cost(COVER),
    )()
    sums = pl.pallas_call(
        lambda *refs: project_kernel(
            *refs, kv_count=kv_count, own_seqs=own_seqs, gate_count=gate_count
        ),
        name="project",
        in_specs=[VMEM] + [HBM] * 8,
        out_specs=[VMEM] * kv_count,
        out_shape=[jax.ShapeDtypeStruct((own_seqs, packed), F32)] * kv_count,
        scratch_shapes=[
            pltpu.VMEM((rows, width), BF16),
            pltpu.VMEM((1, width), F32),
            pltpu.VMEM((4, width, cols), BF16),
            pltpu.VMEM((2, gate_count, width), BF16),
            pltpu.VMEM((kv_count, own_seqs, packed), F32),
            pltpu.SemaphoreType.DMA((8,)),
        ],
        compiler_params=grant(6),
        cost_estimate=cost(COVER),
    )(
        mark,
        tokens,
        pre_gain.reshape(1, width),
        query_weight,
        key_weight,
        value_weight,
        outgate_weight,
        input_gate_weight.T,
        forget_gate_weight.T,
    )
    sums = [sums[0]] + [xor_swap(sums[step], step, kv_count) for step in range(1, kv_count)]
    cell_args = (
        cache_input.transpose(0, 2, 1),
        cache_forget.transpose(0, 2, 1),
        lengths.reshape(1, own_seqs),
        state_norm,
        state_max,
        head_gain.reshape(1, cols),
        cache_keys,
        state_matrix,
        cache_values,
    )
    packet = pl.pallas_call(
        lambda *refs: cell_kernel(
            *refs,
            kv_count=kv_count,
            model_width=model_width,
            head_count=head_count,
            gate_count=gate_count,
        ),
        name="cell",
        in_specs=[VMEM] * kv_count + [HBM] * 9,
        out_specs=VMEM,
        out_shape=jax.ShapeDtypeStruct((own_seqs, cols), BF16),
        scratch_shapes=[pltpu.VMEM(x.shape, x.dtype) for x in cell_args]
        + [pltpu.SemaphoreType.DMA((9,))],
        compiler_params=grant(6),
        cost_estimate=cost(COVER),
    )(*sums, *cell_args)
    packets = [packet] + [xor_swap(packet, step, kv_count) for step in range(1, kv_count)]
    product = pl.pallas_call(
        lambda *refs: mix_kernel(*refs, kv_count=kv_count),
        name="mix",
        in_specs=[VMEM] * (kv_count + 1),
        out_specs=VMEM,
        out_shape=jax.ShapeDtypeStruct((rows, width), BF16),
        scratch_shapes=[pltpu.VMEM((kv_count, own_seqs, cols), F32)],
        compiler_params=grant(4),
        cost_estimate=cost(COVER),
    )(*packets, out_weight)
    mixed = product.astype(F32)
    for step in range(1, tp_count):
        swap = [(i, (i + step) % tp_count) for i in range(tp_count)]
        mixed = mixed + lax.ppermute(product, "tp", swap).astype(F32)
    residual = (tokens.astype(F32) + mixed).astype(BF16)
    blocks = [residual] + [xor_swap(residual, step, kv_count) for step in range(1, kv_count)]
    shares = pl.pallas_call(
        lambda *refs: mixer_kernel(*refs, kv_count=kv_count, model_width=model_width),
        name="mixer",
        in_specs=[VMEM] * (kv_count + 4),
        out_specs=VMEM,
        out_shape=jax.ShapeDtypeStruct((group, rows, narrow), F32),
        scratch_shapes=[pltpu.VMEM((kv_count, rows, width), F32)],
        compiler_params=grant(4),
    )(*blocks, mixer_gain.reshape(1, model_width), gate_weight.T, up_weight.T, down_weight)
    shares = lax.all_to_all(shares, ("kv", "tp"), 0, 0, tiled=True)
    own = lax.dynamic_slice_in_dim(residual, lax.axis_index("tp") * narrow, narrow, 1).astype(F32)
    return (own + jnp.sum(shares, axis=0)).astype(BF16)


def per_device(
    tokens,
    pre_gain,
    query_weight,
    key_weight,
    value_weight,
    outgate_weight,
    input_gate_weight,
    forget_gate_weight,
    cache_keys,
    cache_values,
    cache_input,
    cache_forget,
    lengths,
    state_matrix,
    state_norm,
    state_max,
    head_gain,
    out_weight,
    mixer_gain,
    gate_weight,
    up_weight,
    down_weight,
):
    col_width = tokens.shape[1]
    own_seqs = cache_keys.shape[0]
    block_len = cache_keys.shape[1]
    head_count = state_max.shape[1]
    head_size = state_norm.shape[2]
    shard_index = lax.axis_index("kv")
    half_index = lax.axis_index("tp")
    kv_count = lax.axis_size("kv")
    model_width = col_width * kv_count
    token_values = tokens.astype(jnp.float32)
    squares = jnp.sum(token_values * token_values, axis=1)
    normed = (token_values * pre_gain[None, :]).astype(jnp.bfloat16)
    corner = (shard_index * col_width, half_index * head_count)
    gate_pair = jnp.concatenate(
        [
            lax.dynamic_slice(input_gate_weight, corner, (col_width, head_count)),
            lax.dynamic_slice(forget_gate_weight, corner, (col_width, head_count)),
        ],
        axis=1,
    )

    def product(weight):
        return jnp.dot(normed, weight, preferred_element_type=jnp.float32)

    query_term = product(query_weight)
    key_term = product(key_weight)
    value_term = product(value_weight)
    outgate_term = product(outgate_weight)
    gate_term = product(gate_pair)
    square_totals = lax.psum(squares, "kv")
    query_sum, key_sum, value_sum, outgate_sum, gate_sum = (
        lax.psum_scatter(query_term, "kv", scatter_dimension=0, tiled=True),
        lax.psum_scatter(key_term, "kv", scatter_dimension=0, tiled=True),
        lax.psum_scatter(value_term, "kv", scatter_dimension=0, tiled=True),
        lax.psum_scatter(outgate_term, "kv", scatter_dimension=0, tiled=True),
        lax.psum_scatter(gate_term, "kv", scatter_dimension=0, tiled=True),
    )
    own_squares = lax.dynamic_slice_in_dim(square_totals, shard_index * own_seqs, own_seqs, 0)
    scale_first = lax.rsqrt(own_squares / model_width + EPS)[:, None]
    query = (scale_first * query_sum).astype(jnp.bfloat16)
    keys_new = (scale_first * key_sum).astype(jnp.bfloat16)
    values_new = (scale_first * value_sum).astype(jnp.bfloat16)
    outgate = (scale_first * outgate_sum).astype(jnp.bfloat16)
    gate_values = scale_first * gate_sum
    in_gate = gate_values[:, :head_count]
    forget_new = jax.nn.log_sigmoid(gate_values[:, head_count:])
    query_heads = query.reshape(own_seqs, head_count, head_size)
    key_heads = keys_new.reshape(own_seqs, head_count, head_size)
    value_heads = values_new.reshape(own_seqs, head_count, head_size)
    cached_keys = cache_keys.reshape(own_seqs, block_len, head_count, head_size)
    cached_values = cache_values.reshape(own_seqs, block_len, head_count, head_size)
    inv_root = head_size ** (-0.5)
    live_mask = (lax.broadcasted_iota(jnp.int32, (own_seqs, block_len), 1) < lengths[:, None])[
        :, :, None
    ]
    forget_live = jnp.where(live_mask, cache_forget, jnp.float32(0.0))
    running = jnp.cumsum(forget_live, axis=1)
    total_log = running[:, -1, :] + forget_new
    weight_log = jnp.where(live_mask, total_log[:, None, :] - running + cache_input, -jnp.inf)
    state_log = total_log + state_max
    peak_log = jnp.maximum(jnp.maximum(state_log, in_gate), jnp.max(weight_log, axis=1))
    key_dots = (
        jnp.einsum("shd,slhd->slh", query_heads, cached_keys, preferred_element_type=jnp.float32)
        * inv_root
    )
    block_scores = jnp.exp(weight_log - peak_log[:, None, :]) * key_dots
    query_scaled = query_heads.astype(jnp.float32) * inv_root
    self_score = jnp.exp(in_gate - peak_log) * jnp.sum(
        query_scaled * key_heads.astype(jnp.float32), axis=2
    )
    carried = jnp.exp(state_log - peak_log)
    block_weights = block_scores.astype(jnp.bfloat16)
    memory_read = jnp.einsum(
        "shvd,shd->shv", state_matrix, query_scaled, precision=lax.Precision.HIGHEST
    )
    norm_read = jnp.einsum("shd,shd->sh", state_norm, query_scaled, precision=lax.Precision.HIGHEST)
    numerator = (
        carried[:, :, None] * memory_read
        + jnp.einsum(
            "slh,slhd->shd", block_weights, cached_values, preferred_element_type=jnp.float32
        )
        + self_score[:, :, None] * value_heads.astype(jnp.float32)
    )
    denominator = carried * norm_read + jnp.sum(block_scores, axis=1) + self_score
    hidden = numerator / jnp.maximum(jnp.abs(denominator), 1.0)[:, :, None]
    mixed_heads = (
        hidden.reshape(own_seqs, head_count * head_size)
        * head_gain[None, :]
        * jax.nn.sigmoid(outgate.astype(jnp.float32))
    ).astype(jnp.bfloat16)
    mix_terms = jnp.dot(
        lax.all_gather(mixed_heads, "kv", axis=0, tiled=True),
        out_weight,
        preferred_element_type=jnp.float32,
    )
    mix_sum = lax.psum_scatter(
        mix_terms.astype(jnp.bfloat16), "tp", scatter_dimension=1, tiled=True
    ).astype(jnp.float32)
    narrow = mix_sum.shape[1]
    residual = (
        lax.dynamic_slice_in_dim(token_values, half_index * narrow, narrow, 1) + mix_sum
    ).astype(jnp.bfloat16)
    piece_wide = lax.all_gather(residual, ("kv", "tp"), axis=1, tiled=True).astype(jnp.float32)
    normed_piece = (piece_wide * mixer_gain[None, :]).astype(jnp.bfloat16)
    gate_acc = jnp.dot(normed_piece, gate_weight, preferred_element_type=jnp.float32)
    up_acc = jnp.dot(normed_piece, up_weight, preferred_element_type=jnp.float32)
    sum_squares = jnp.sum(piece_wide * piece_wide, axis=1)
    gate_acc, up_acc, sum_squares = (gate_acc, up_acc, sum_squares)
    scale_mid = lax.rsqrt(sum_squares / model_width + EPS)[:, None]
    hidden_units = (jax.nn.silu(scale_mid * gate_acc) * (scale_mid * up_acc)).astype(jnp.bfloat16)
    summed = lax.psum_scatter(
        lax.dot_general(
            down_weight, hidden_units, (((0,), (1,)), ((), ())), preferred_element_type=jnp.float32
        ),
        ("kv", "tp"),
        scatter_dimension=0,
        tiled=True,
    )
    mixer_out = summed.T
    return (residual.astype(jnp.float32) + mixer_out).astype(jnp.bfloat16)


def solution(mesh):
    in_specs = (
        P("dp", "kv"),
        P("kv"),
        P("kv", "tp"),
        P("kv", "tp"),
        P("kv", "tp"),
        P("kv", "tp"),
        P(),
        P(),
        P(("dp", "kv"), None, "tp"),
        P(("dp", "kv"), None, "tp"),
        P(("dp", "kv"), None, "tp"),
        P(("dp", "kv"), None, "tp"),
        P(("dp", "kv")),
        P(("dp", "kv"), "tp", None, None),
        P(("dp", "kv"), "tp", None),
        P(("dp", "kv"), "tp"),
        P("tp"),
        P("tp", "kv"),
        P(),
        P(None, ("kv", "tp")),
        P(None, ("kv", "tp")),
        P(("kv", "tp"), None),
    )
    out_specs = P("dp", ("kv", "tp"))
    kv_count = mesh.shape["kv"]

    def aligned(*args):
        width, cols = args[2].shape
        width, cols = width // kv_count, cols // mesh.shape["tp"]
        narrow = width // mesh.shape["tp"]
        return (
            kv_count & (kv_count - 1) == 0
            and kv_count <= 8
            and width == cols
            and narrow % LANES == 0
        )

    def run(*args):
        body = aligned_device if aligned(*args) else per_device
        return sharded(body)(*args)

    def sharded(body):
        return jax.shard_map(
            body, mesh=mesh, in_specs=in_specs, out_specs=out_specs, check_vma=False
        )

    return run
```

```python
import jax
import jax.numpy as jnp
from jax import lax
from jax.experimental import pallas as pl
from jax.experimental.pallas import tpu as pltpu
from jax.sharding import PartitionSpec as P

EPS = 1e-06
LANES = 128
PIECES = 3
COVER = 6_000_000_000
VMEM = pl.BlockSpec(memory_space=pltpu.VMEM)
HBM = pl.BlockSpec(memory_space=pltpu.HBM)
F32 = jnp.float32
BF16 = jnp.bfloat16


def dot(a, b, dims=((1,), (0,))):
    return lax.dot_general(a, b, (dims, ((), ())), preferred_element_type=F32)


def fetch(sources, targets, sems):
    copies = [
        pltpu.make_async_copy(source, target, sems.at[n])
        for n, (source, target) in enumerate(zip(sources, targets))
    ]
    for copy in copies:
        copy.start()
    return copies


def cost(flops):
    return pl.CostEstimate(flops=flops, bytes_accessed=0, transcendentals=0)


def grant(mebibytes):
    return pltpu.CompilerParams(vmem_limit_bytes=mebibytes * 2**20)


def xor_swap(value, step, count):
    return lax.ppermute(value, "kv", [(i, i ^ step) for i in range(count)])


def marker_kernel(mark, *, lane_at):
    lane = lax.broadcasted_iota(jnp.int32, mark.shape, 1)
    mark[...] = jnp.where(lane == lane_at, 1.0, 0.0)


def project_kernel(
    mark, tokens, gain, wq, wk, wv, wo, wi, wf, *rest, kv_count, own_seqs, gate_count
):
    outs = rest[:kv_count]
    token_buf, gain_buf, bufs, gate_bufs, acc, sems = rest[kv_count:]
    rows, width = tokens.shape
    cols = wq.shape[1]
    me = lax.axis_index("kv")
    here = pl.ds(pl.multiple_of(me * width, width), width)
    sources = (tokens, gain, wi.at[:, here], wf.at[:, here], wq, wk, wv, wo)
    targets = (token_buf, gain_buf, gate_bufs.at[0], gate_bufs.at[1], *[bufs.at[n] for n in range(4)])
    copies = fetch(sources, targets, sems)
    copies[0].wait()
    copies[1].wait()
    values = token_buf[...].astype(F32)
    squares = jnp.sum(values * values, axis=1, keepdims=True)
    normed = (values * gain_buf[...]).astype(BF16)
    extra = mark[...] * squares

    def put(start, part):
        for k in range(kv_count):
            acc[k, :, start : start + part.shape[1]] = part[k * own_seqs : (k + 1) * own_seqs, :]

    put(4 * cols, extra)
    for n in range(4):
        copies[4 + n].wait()
        put(n * cols, dot(normed, bufs[n]))
    for n in range(2):
        copies[2 + n].wait()
        put(4 * cols + n * gate_count, dot(normed, gate_bufs[n], ((1,), (1,))))
    for step in range(kv_count):
        block = acc[me ^ step]
        outs[step][:, : 4 * cols] = block[:, : 4 * cols].astype(BF16)
        rest = block[:, 4 * cols :]
        for n in range(PIECES):
            piece = rest.astype(BF16)
            outs[step][:, 4 * cols + n * LANES : 4 * cols + (n + 1) * LANES] = piece
            rest = rest - piece.astype(F32)


def cell_kernel(
    *refs, kv_count, model_width, head_count, gate_count
):
    parts = refs[:kv_count]
    sources = refs[kv_count : kv_count + 9]
    out = refs[kv_count + 9]
    buffers = refs[kv_count + 10 : kv_count + 19]
    copies = fetch(sources, buffers, refs[kv_count + 19])
    (cache_input, cache_forget, lengths, norm, peak, gain, keys, state, values) = buffers
    own_seqs, block_len, cols = keys.shape
    head_size = cols // head_count
    half = lax.axis_index("tp")
    inv_root = head_size ** (-0.5)
    total = parts[0][...].astype(F32)
    for part in parts[1:]:
        total = total + part[...].astype(F32)
    extra = total[:, 4 * cols : 4 * cols + LANES]
    for n in range(1, PIECES):
        extra = extra + total[:, 4 * cols + n * LANES : 4 * cols + (n + 1) * LANES]
    squares = extra[:, 2 * gate_count : 2 * gate_count + 1]
    scale = lax.rsqrt(squares / model_width + EPS)
    query, key_new, value_new, outgate = [
        (scale * total[:, n * cols : (n + 1) * cols]).astype(BF16) for n in range(4)
    ]
    gates = scale * extra

    lane_head = lax.broadcasted_iota(jnp.int32, (head_count, cols), 1) // head_size
    own_lane = lane_head == lax.broadcasted_iota(jnp.int32, (head_count, cols), 0)
    upper = (
        lax.broadcasted_iota(jnp.int32, (block_len, block_len), 0)
        <= lax.broadcasted_iota(jnp.int32, (block_len, block_len), 1)
    ).astype(F32)
    position = lax.broadcasted_iota(jnp.int32, (head_count, block_len), 1)

    def column(row, start):
        shape = (head_count, row.shape[1])
        at = lax.broadcasted_iota(jnp.int32, shape, 0) + start
        picked = jnp.where(lax.broadcasted_iota(jnp.int32, shape, 1) == at, row, 0.0)
        return jnp.sum(picked, axis=1, keepdims=True)


    def spread(per_head):
        return jnp.sum(jnp.where(own_lane, per_head, 0.0), axis=0, keepdims=True)

    for copy in copies:
        copy.wait()
    for s in range(own_seqs):
        live = position < lengths[:, s : s + 1]
        forget_live = jnp.where(live, cache_forget[s], 0.0)
        running = lax.dot_general(
            forget_live,
            upper,
            (((1,), (0,)), ((), ())),
            precision=lax.Precision.HIGHEST,
            preferred_element_type=F32,
        )
        gates_s = gates[s : s + 1]
        gate_s = column(gates_s, half * head_count)
        forget_new = jax.nn.log_sigmoid(column(gates_s, gate_count + half * head_count))
        total_log = running[:, block_len - 1 : block_len] + forget_new
        weight_log = jnp.where(live, total_log - running + cache_input[s], -jnp.inf)
        state_log = total_log + column(peak[s : s + 1], 0)
        peak_log = jnp.maximum(
            jnp.maximum(state_log, gate_s), jnp.max(weight_log, axis=1, keepdims=True)
        )
        query_s = query[s : s + 1].astype(F32)
        query_rows = jnp.where(own_lane, query_s, 0.0)
        key_dots = dot(query_rows.astype(BF16), keys[s], ((1,), (1,))) * inv_root
        scores = jnp.exp(weight_log - peak_log) * key_dots
        query_rows = query_rows * inv_root
        self_dot = jnp.sum(query_rows * key_new[s : s + 1].astype(F32), axis=1, keepdims=True)
        read = dot(scores.astype(BF16), values[s])
        read = jnp.sum(jnp.where(own_lane, read, 0.0), axis=0, keepdims=True)
        memory, norm_dot = [], []
        for h in range(head_count):
            at = slice(h * head_size, (h + 1) * head_size)
            matrix = state[s, h]
            high = matrix.astype(BF16)
            low = (matrix - high.astype(F32)).astype(BF16)
            query_h = query_s[:, at].astype(BF16)
            memory.append(dot(query_h, high, ((1,), (1,))) + dot(query_h, low, ((1,), (1,))))
            norm_dot.append(
                jnp.sum(query_s[:, at] * norm[s, h : h + 1, :], axis=1, keepdims=True)
            )
        memory = jnp.concatenate(memory, axis=1) * inv_root
        norm_dot = jnp.concatenate(norm_dot, axis=0) * inv_root
        self_score = jnp.exp(gate_s - peak_log) * self_dot
        carried = jnp.exp(state_log - peak_log)
        numerator = (
            spread(carried) * memory + read + spread(self_score) * value_new[s : s + 1].astype(F32)
        )
        denominator = carried * norm_dot + jnp.sum(scores, axis=1, keepdims=True) + self_score
        hidden = numerator / spread(jnp.maximum(jnp.abs(denominator), 1.0))
        gated = hidden * gain[...] * jax.nn.sigmoid(outgate[s : s + 1].astype(F32))
        out[s : s + 1, :] = gated.astype(BF16)


def mix_kernel(*refs, kv_count):
    parts = refs[:kv_count]
    weight, product, ordered = refs[kv_count:]
    me = lax.axis_index("kv")
    for step in range(kv_count):
        ordered[me ^ step] = parts[step][...].astype(F32)
    heads = jnp.concatenate([ordered[k] for k in range(kv_count)], axis=0).astype(BF16)
    product[...] = dot(heads, weight[...]).astype(BF16)


def mixer_kernel(*refs, kv_count, model_width):
    parts = refs[:kv_count]
    gain, wg, wu, wd, sent, ordered = refs[kv_count:]
    rows, width = parts[0].shape
    narrow = sent.shape[2]
    me = lax.axis_index("kv")
    squares = jnp.zeros((rows, 1), F32)
    for step in range(kv_count):
        wide = parts[step][...].astype(F32)
        squares = squares + jnp.sum(wide * wide, axis=1, keepdims=True)
        ordered[me ^ step] = wide
    normed = jnp.concatenate(
        [ordered[k] * gain[:, k * width : (k + 1) * width] for k in range(kv_count)], axis=1
    ).astype(BF16)
    scale = lax.rsqrt(squares / model_width + EPS)
    gate = scale * dot(normed, wg[...], ((1,), (1,)))
    up = scale * dot(normed, wu[...], ((1,), (1,)))
    units = (jax.nn.silu(gate) * up).astype(BF16)
    for k in range(sent.shape[0]):
        sent[k] = dot(units, wd[:, k * narrow : (k + 1) * narrow])


def aligned_device(
    tokens,
    pre_gain,
    query_weight,
    key_weight,
    value_weight,
    outgate_weight,
    input_gate_weight,
    forget_gate_weight,
    cache_keys,
    cache_values,
    cache_input,
    cache_forget,
    lengths,
    state_matrix,
    state_norm,
    state_max,
    head_gain,
    out_weight,
    mixer_gain,
    gate_weight,
    up_weight,
    down_weight,
):
    kv_count = lax.axis_size("kv")
    tp_count = lax.axis_size("tp")
    rows, width = tokens.shape
    own_seqs = cache_keys.shape[0]
    cols = query_weight.shape[1]
    head_count = state_max.shape[1]
    gate_count = input_gate_weight.shape[1]
    model_width = width * kv_count
    group = kv_count * tp_count
    narrow = width // tp_count
    packed = 4 * cols + LANES
    mark = pl.pallas_call(
        lambda ref: marker_kernel(ref, lane_at=2 * gate_count),
        name="marker",
        out_specs=VMEM,
        out_shape=jax.ShapeDtypeStruct((rows, LANES), F32),
        compiler_params=grant(1),
        cost_estimate=cost(COVER),
    )()
    sums = pl.pallas_call(
        lambda *refs: project_kernel(
            *refs, kv_count=kv_count, own_seqs=own_seqs, gate_count=gate_count
        ),
        name="project",
        in_specs=[VMEM] + [HBM] * 8,
        out_specs=[VMEM] * kv_count,
        out_shape=[jax.ShapeDtypeStruct((own_seqs, packed + (PIECES - 1) * LANES), BF16)] * kv_count,
        scratch_shapes=[
            pltpu.VMEM((rows, width), BF16),
            pltpu.VMEM((1, width), F32),
            pltpu.VMEM((4, width, cols), BF16),
            pltpu.VMEM((2, gate_count, width), BF16),
            pltpu.VMEM((kv_count, own_seqs, packed), F32),
            pltpu.SemaphoreType.DMA((8,)),
        ],
        compiler_params=grant(6),
        cost_estimate=cost(COVER),
    )(
        mark,
        tokens,
        pre_gain.reshape(1, width),
        query_weight,
        key_weight,
        value_weight,
        outgate_weight,
        input_gate_weight.T,
        forget_gate_weight.T,
    )
    sums = [sums[0]] + [xor_swap(sums[step], step, kv_count) for step in range(1, kv_count)]
    cell_args = (
        cache_input.transpose(0, 2, 1),
        cache_forget.transpose(0, 2, 1),
        lengths.reshape(1, own_seqs),
        state_norm,
        state_max,
        head_gain.reshape(1, cols),
        cache_keys,
        state_matrix,
        cache_values,
    )
    packet = pl.pallas_call(
        lambda *refs: cell_kernel(
            *refs,
            kv_count=kv_count,
            model_width=model_width,
            head_count=head_count,
            gate_count=gate_count,
        ),
        name="cell",
        in_specs=[VMEM] * kv_count + [HBM] * 9,
        out_specs=VMEM,
        out_shape=jax.ShapeDtypeStruct((own_seqs, cols), BF16),
        scratch_shapes=[pltpu.VMEM(x.shape, x.dtype) for x in cell_args]
        + [pltpu.SemaphoreType.DMA((9,))],
        compiler_params=grant(6),
        cost_estimate=cost(COVER),
    )(*sums, *cell_args)
    packets = [packet] + [xor_swap(packet, step, kv_count) for step in range(1, kv_count)]
    product = pl.pallas_call(
        lambda *refs: mix_kernel(*refs, kv_count=kv_count),
        name="mix",
        in_specs=[VMEM] * (kv_count + 1),
        out_specs=VMEM,
        out_shape=jax.ShapeDtypeStruct((rows, width), BF16),
        scratch_shapes=[pltpu.VMEM((kv_count, own_seqs, cols), F32)],
        compiler_params=grant(4),
        cost_estimate=cost(COVER),
    )(*packets, out_weight)
    mixed = product.astype(F32)
    for step in range(1, tp_count):
        swap = [(i, (i + step) % tp_count) for i in range(tp_count)]
        mixed = mixed + lax.ppermute(product, "tp", swap).astype(F32)
    residual = (tokens.astype(F32) + mixed).astype(BF16)
    blocks = [residual] + [xor_swap(residual, step, kv_count) for step in range(1, kv_count)]
    shares = pl.pallas_call(
        lambda *refs: mixer_kernel(*refs, kv_count=kv_count, model_width=model_width),
        name="mixer",
        in_specs=[VMEM] * (kv_count + 4),
        out_specs=VMEM,
        out_shape=jax.ShapeDtypeStruct((group, rows, narrow), F32),
        scratch_shapes=[pltpu.VMEM((kv_count, rows, width), F32)],
        compiler_params=grant(4),
    )(*blocks, mixer_gain.reshape(1, model_width), gate_weight.T, up_weight.T, down_weight)
    shares = lax.all_to_all(shares, ("kv", "tp"), 0, 0, tiled=True)
    own = lax.dynamic_slice_in_dim(residual, lax.axis_index("tp") * narrow, narrow, 1).astype(F32)
    return (own + jnp.sum(shares, axis=0)).astype(BF16)


def per_device(
    tokens,
    pre_gain,
    query_weight,
    key_weight,
    value_weight,
    outgate_weight,
    input_gate_weight,
    forget_gate_weight,
    cache_keys,
    cache_values,
    cache_input,
    cache_forget,
    lengths,
    state_matrix,
    state_norm,
    state_max,
    head_gain,
    out_weight,
    mixer_gain,
    gate_weight,
    up_weight,
    down_weight,
):
    col_width = tokens.shape[1]
    own_seqs = cache_keys.shape[0]
    block_len = cache_keys.shape[1]
    head_count = state_max.shape[1]
    head_size = state_norm.shape[2]
    shard_index = lax.axis_index("kv")
    half_index = lax.axis_index("tp")
    kv_count = lax.axis_size("kv")
    model_width = col_width * kv_count
    token_values = tokens.astype(jnp.float32)
    squares = jnp.sum(token_values * token_values, axis=1)
    normed = (token_values * pre_gain[None, :]).astype(jnp.bfloat16)
    corner = (shard_index * col_width, half_index * head_count)
    gate_pair = jnp.concatenate(
        [
            lax.dynamic_slice(input_gate_weight, corner, (col_width, head_count)),
            lax.dynamic_slice(forget_gate_weight, corner, (col_width, head_count)),
        ],
        axis=1,
    )

    def product(weight):
        return jnp.dot(normed, weight, preferred_element_type=jnp.float32)

    query_term = product(query_weight)
    key_term = product(key_weight)
    value_term = product(value_weight)
    outgate_term = product(outgate_weight)
    gate_term = product(gate_pair)
    square_totals = lax.psum(squares, "kv")
    query_sum, key_sum, value_sum, outgate_sum, gate_sum = (
        lax.psum_scatter(query_term, "kv", scatter_dimension=0, tiled=True),
        lax.psum_scatter(key_term, "kv", scatter_dimension=0, tiled=True),
        lax.psum_scatter(value_term, "kv", scatter_dimension=0, tiled=True),
        lax.psum_scatter(outgate_term, "kv", scatter_dimension=0, tiled=True),
        lax.psum_scatter(gate_term, "kv", scatter_dimension=0, tiled=True),
    )
    own_squares = lax.dynamic_slice_in_dim(square_totals, shard_index * own_seqs, own_seqs, 0)
    scale_first = lax.rsqrt(own_squares / model_width + EPS)[:, None]
    query = (scale_first * query_sum).astype(jnp.bfloat16)
    keys_new = (scale_first * key_sum).astype(jnp.bfloat16)
    values_new = (scale_first * value_sum).astype(jnp.bfloat16)
    outgate = (scale_first * outgate_sum).astype(jnp.bfloat16)
    gate_values = scale_first * gate_sum
    in_gate = gate_values[:, :head_count]
    forget_new = jax.nn.log_sigmoid(gate_values[:, head_count:])
    query_heads = query.reshape(own_seqs, head_count, head_size)
    key_heads = keys_new.reshape(own_seqs, head_count, head_size)
    value_heads = values_new.reshape(own_seqs, head_count, head_size)
    cached_keys = cache_keys.reshape(own_seqs, block_len, head_count, head_size)
    cached_values = cache_values.reshape(own_seqs, block_len, head_count, head_size)
    inv_root = head_size ** (-0.5)
    live_mask = (lax.broadcasted_iota(jnp.int32, (own_seqs, block_len), 1) < lengths[:, None])[
        :, :, None
    ]
    forget_live = jnp.where(live_mask, cache_forget, jnp.float32(0.0))
    running = jnp.cumsum(forget_live, axis=1)
    total_log = running[:, -1, :] + forget_new
    weight_log = jnp.where(live_mask, total_log[:, None, :] - running + cache_input, -jnp.inf)
    state_log = total_log + state_max
    peak_log = jnp.maximum(jnp.maximum(state_log, in_gate), jnp.max(weight_log, axis=1))
    key_dots = (
        jnp.einsum("shd,slhd->slh", query_heads, cached_keys, preferred_element_type=jnp.float32)
        * inv_root
    )
    block_scores = jnp.exp(weight_log - peak_log[:, None, :]) * key_dots
    query_scaled = query_heads.astype(jnp.float32) * inv_root
    self_score = jnp.exp(in_gate - peak_log) * jnp.sum(
        query_scaled * key_heads.astype(jnp.float32), axis=2
    )
    carried = jnp.exp(state_log - peak_log)
    block_weights = block_scores.astype(jnp.bfloat16)
    memory_read = jnp.einsum(
        "shvd,shd->shv", state_matrix, query_scaled, precision=lax.Precision.HIGHEST
    )
    norm_read = jnp.einsum("shd,shd->sh", state_norm, query_scaled, precision=lax.Precision.HIGHEST)
    numerator = (
        carried[:, :, None] * memory_read
        + jnp.einsum(
            "slh,slhd->shd", block_weights, cached_values, preferred_element_type=jnp.float32
        )
        + self_score[:, :, None] * value_heads.astype(jnp.float32)
    )
    denominator = carried * norm_read + jnp.sum(block_scores, axis=1) + self_score
    hidden = numerator / jnp.maximum(jnp.abs(denominator), 1.0)[:, :, None]
    mixed_heads = (
        hidden.reshape(own_seqs, head_count * head_size)
        * head_gain[None, :]
        * jax.nn.sigmoid(outgate.astype(jnp.float32))
    ).astype(jnp.bfloat16)
    mix_terms = jnp.dot(
        lax.all_gather(mixed_heads, "kv", axis=0, tiled=True),
        out_weight,
        preferred_element_type=jnp.float32,
    )
    mix_sum = lax.psum_scatter(
        mix_terms.astype(jnp.bfloat16), "tp", scatter_dimension=1, tiled=True
    ).astype(jnp.float32)
    narrow = mix_sum.shape[1]
    residual = (
        lax.dynamic_slice_in_dim(token_values, half_index * narrow, narrow, 1) + mix_sum
    ).astype(jnp.bfloat16)
    piece_wide = lax.all_gather(residual, ("kv", "tp"), axis=1, tiled=True).astype(jnp.float32)
    normed_piece = (piece_wide * mixer_gain[None, :]).astype(jnp.bfloat16)
    gate_acc = jnp.dot(normed_piece, gate_weight, preferred_element_type=jnp.float32)
    up_acc = jnp.dot(normed_piece, up_weight, preferred_element_type=jnp.float32)
    sum_squares = jnp.sum(piece_wide * piece_wide, axis=1)
    gate_acc, up_acc, sum_squares = (gate_acc, up_acc, sum_squares)
    scale_mid = lax.rsqrt(sum_squares / model_width + EPS)[:, None]
    hidden_units = (jax.nn.silu(scale_mid * gate_acc) * (scale_mid * up_acc)).astype(jnp.bfloat16)
    summed = lax.psum_scatter(
        lax.dot_general(
            down_weight, hidden_units, (((0,), (1,)), ((), ())), preferred_element_type=jnp.float32
        ),
        ("kv", "tp"),
        scatter_dimension=0,
        tiled=True,
    )
    mixer_out = summed.T
    return (residual.astype(jnp.float32) + mixer_out).astype(jnp.bfloat16)


def solution(mesh):
    in_specs = (
        P("dp", "kv"),
        P("kv"),
        P("kv", "tp"),
        P("kv", "tp"),
        P("kv", "tp"),
        P("kv", "tp"),
        P(),
        P(),
        P(("dp", "kv"), None, "tp"),
        P(("dp", "kv"), None, "tp"),
        P(("dp", "kv"), None, "tp"),
        P(("dp", "kv"), None, "tp"),
        P(("dp", "kv")),
        P(("dp", "kv"), "tp", None, None),
        P(("dp", "kv"), "tp", None),
        P(("dp", "kv"), "tp"),
        P("tp"),
        P("tp", "kv"),
        P(),
        P(None, ("kv", "tp")),
        P(None, ("kv", "tp")),
        P(("kv", "tp"), None),
    )
    out_specs = P("dp", ("kv", "tp"))
    kv_count = mesh.shape["kv"]

    def aligned(*args):
        width, cols = args[2].shape
        width, cols = width // kv_count, cols // mesh.shape["tp"]
        narrow = width // mesh.shape["tp"]
        return (
            kv_count & (kv_count - 1) == 0
            and kv_count <= 8
            and width == cols
            and narrow % LANES == 0
        )

    def run(*args):
        body = aligned_device if aligned(*args) else per_device
        return sharded(body)(*args)

    def sharded(body):
        return jax.shard_map(
            body, mesh=mesh, in_specs=in_specs, out_specs=out_specs, check_vma=False
        )

    return run
```
